512 devices in a mesh: fs: 64 (over z, y), tp: 8 (over x, core).
Axes of the slice: x: 4, y: 4, z: 16, core: 2. Of those that a mesh axis runs over, the one named last changes fastest.
Arguments:
- inputs: bfloat16 [16384, 2048], P('fs'), may hold values from -6 to 6
- query_cot: bfloat16 [16384, 1024], P('fs', 'tp'), may hold values from -0.046875 to 0.046875
- query_basis: bfloat16 [2048, 256], P('fs'), may hold values from -0.125 to 0.125
- query_master: float32 [2048, 1024], P('fs', 'tp'), may hold values from -3 to 3
- query_first: float32 [256, 1024], P('fs', 'tp'), may hold values from -4 to 4
- query_second: float32 [256, 1024], P('fs', 'tp'), may hold values from 0.02 to 4
Outputs:
- query_step: float32 [2048, 1024], P('fs', 'tp')
- query_first_new: float32 [256, 1024], P('fs', 'tp')
- query_second_new: float32 [256, 1024], P('fs', 'tp')
- query_copy: bfloat16 [2048, 1024], P('fs', 'tp')
The draws below stay inside these ranges and needn't reach their ends.
All inputs are finite; a program needn't handle non-finite values.
Results may differ from the reference program's by a relative error of at most 0.0011.
Values may be sent and summed in bfloat16 or wider, within the bound.
A program may use at most 64 MiB of HBM per device.

```python
import math
import jax
import jax.numpy as jnp
from jax import lax

D = 2048
HEADS = 8
DQK = 128
RANK = 256
TOK_DEV = 256
TOKENS = 16384
NQ = 1024
N_FS = 64


def levels(key, extent, pieces, least, top_value):
    def one(position, blocks):
        heights = jax.random.uniform(jax.random.fold_in(jax.random.fold_in(key, 6), position), (blocks,), jnp.float32, least / len(pieces), top_value / len(pieces))
        return jnp.repeat(jnp.exp(heights), extent[position] // blocks).reshape((-1,) + (1,) * (len(extent) - position - 1))

    level = one(*pieces[0])
    for cut in pieces[1:]:
        level = level * one(*cut)
    return level


def scatter_about(rng, dims, spread, reach, pieces=(), dtype=jnp.bfloat16):
    values = jax.random.normal(rng, dims, jnp.float32) * spread
    if len(pieces) > 0:
        values = levels(rng, dims, pieces, -0.22, 0.18) * values
    return jnp.clip(values, min=-reach, max=reach).astype(dtype)


def setup_inputs(seed: int = 0) -> dict:
    streams_of = jax.random.split(jax.random.key(seed), 7)
    return {
        "inputs": scatter_about(streams_of[0], (TOKENS, D), 1.0, 6.0, ((0, 64),)),
        "query_cot": scatter_about(streams_of[1], (TOKENS, NQ), (1.0 / (TOK_DEV * N_FS) ** 0.5), 0.046875, ((0, 64), (1, 8))),
        "query_basis": scatter_about(streams_of[2], (D, RANK), D ** -0.5, 0.125, ((0, 64),)),
        "query_master": scatter_about(streams_of[3], (D, NQ), 0.5, 3.0, ((0, 64), (1, 8)), jnp.float32),
        "query_first": scatter_about(streams_of[4], (RANK, NQ), 1.0, 4.0, ((0, 64), (1, 8)), jnp.float32),
        "query_second": jnp.clip(jnp.exp(math.log(4.0) - 5.2983174 * jax.random.uniform(streams_of[5], (RANK, NQ), jnp.float32) ** levels(streams_of[5], (RANK, NQ), ((0, 64), (1, 8)), -0.2, 0.2)), 0.02, 4.0),
    }


def moments(first, second, low_grad):
    first_new = 0.8 * first + 0.2 * low_grad
    second_new = 0.9 * second + 0.1 * low_grad * low_grad
    return (first_new, second_new, first_new / jnp.sqrt(second_new))

def scaled(update, width):
    shaped = update.reshape(RANK, HEADS, width)
    head_mean = lax.optimization_barrier(jnp.mean(shaped * shaped, axis=(0, 2)))
    whole_mean = jnp.mean(update * update)
    factor = 1.0 / jnp.sqrt(head_mean + whole_mean)
    return (shaped * factor[None, :, None]).reshape(RANK, HEADS * width)

def reference(inputs, query_cot, query_basis, query_master, query_first, query_second):
    gradient = jnp.dot(inputs.T, query_cot, preferred_element_type=jnp.float32)
    basis_wide = query_basis.astype(jnp.float32)
    low_grad = jnp.dot(basis_wide.T, gradient, precision=lax.Precision.HIGHEST)
    first_new, second_new, update = moments(query_first, query_second, low_grad)
    step_full = jnp.dot(basis_wide, scaled(update, DQK), precision=lax.Precision.HIGHEST)
    copy_new = (query_master + step_full).astype(jnp.bfloat16)
    return (step_full, first_new, second_new, copy_new)
```

```python
import jax
import jax.numpy as jnp
from jax import lax
from jax.experimental import pallas as pl
from jax.experimental.pallas import tpu as pltpu
from jax.sharding import Mesh
from jax.sharding import PartitionSpec as P

HEADS = 8
DQK = 128
RANK = 256
NZ, NY, NX, NC = 16, 4, 4, 2
NF, NT = NZ * NY, NX * NC
TP = ("x", "c")
FS = ("z", "y")
MESH = pl.DeviceIdType.MESH


def far_first(k, n):
    h = (k + 1) // 2
    return lax.rem(n // 2 + h * (1 - 2 * lax.rem(k, 2)) + n, n)


def moments(first, second, low_grad):
    first_new = 0.8 * first + 0.2 * low_grad
    second_new = 0.9 * second + 0.1 * low_grad * low_grad
    return (first_new, second_new, first_new / jnp.sqrt(second_new))


def kernel(x_hbm, c_hbm, b_hbm, first_hbm, second_hbm, out_ref,
           x_v, c_v, b_v, first_v, second_v, p_v, s_v, r_v, u_v, t_v, g_v,
           local_sem, send_sem, recv_sem):
    z, y, x, c = (lax.axis_index(a) for a in ("z", "y", "x", "c"))
    f, s = z * NY + y, x * NC + c

    def fs_peer(j):
        return (lax.rem(z + far_first(j // NY, NZ), NZ), lax.rem(y + far_first(lax.rem(j, NY), NY), NY), x, c)

    def tp_peer(j):
        t = lax.rem(s + 1 + j, NT)
        return (z, y, t // NC, lax.rem(t, NC))

    def each(n, do):
        def step(j, carry):
            do(j)
            return carry
        lax.fori_loop(0, n, step, 0)

    def remote(src, dst, phase, peer):
        return pltpu.make_async_remote_copy(src_ref=src, dst_ref=dst, send_sem=send_sem.at[phase],
                                            recv_sem=recv_sem.at[phase], device_id=peer, device_id_type=MESH)

    def wait_for(window, sem):
        pltpu.make_async_copy(window, window, sem).wait()

    barrier = pltpu.get_barrier_semaphore()
    each(NF - 1, lambda j: pl.semaphore_signal(barrier, inc=1, device_id=fs_peer(j), device_id_type=MESH))
    each(NT - 1, lambda j: pl.semaphore_signal(barrier, inc=1, device_id=tp_peer(j), device_id_type=MESH))

    mine = pl.ds(pl.multiple_of(s * DQK, DQK), DQK)
    loads = [pltpu.make_async_copy(src, dst, local_sem.at[i]) for i, (src, dst) in enumerate((
        (b_hbm, b_v), (c_hbm, c_v.at[:, mine]), (x_hbm, x_v), (first_hbm, first_v), (second_hbm, second_v)))]
    for load in loads:
        load.start()

    lane = lax.broadcasted_iota(jnp.int32, (RANK, 128), 1)
    row = lax.broadcasted_iota(jnp.int32, (RANK, 128), 0)
    slot = lane & 31
    to_z = 2 * (slot >> 2) + c
    chosen = row == 16 * to_z + 4 * ((to_z + x) & 3) + (slot & 3)
    select = jnp.where(chosen, 1.0, 0.0).astype(jnp.bfloat16)
    group = lax.broadcasted_iota(jnp.int32, (8, 128), 1) >> 5
    loads[0].wait()
    picked = jnp.dot(b_v[...], select, preferred_element_type=jnp.float32)
    packed = jnp.zeros((8, 128), jnp.float32)
    for j in range(4):
        packed = jnp.where(group == j, picked[8 * j : 8 * j + 8], packed)
    p_v[f] = packed.astype(jnp.bfloat16)
    loads[1].wait()

    pl.semaphore_wait(barrier, NF - 1 + NT - 1)
    each(NF - 1, lambda j: remote(p_v.at[f], p_v.at[f], 0, fs_peer(j)).start())
    each(NT - 1, lambda j: remote(c_v.at[:, mine], c_v.at[:, mine], 1, tp_peer(j)).start())
    for load in loads[2:]:
        load.wait()
    wait_for(p_v.at[pl.ds(0, NF - 1)], recv_sem.at[0])

    blocks = p_v[...].astype(jnp.float32)
    which = lax.broadcasted_iota(jnp.int32, (NF, 4, 8, 128), 1)
    lanes = lax.broadcasted_iota(jnp.int32, (NF, 4, 8, 128), 3) >> 5
    spread = jnp.where(which == lanes, blocks[:, None], 0.0).reshape(NF * 32, 128).astype(jnp.bfloat16)
    wide = jnp.dot(x_v[...], spread, preferred_element_type=jnp.float32).T
    proj = wide[0:32] + wide[32:64] + wide[64:96] + wide[96:128]
    high = proj.astype(jnp.bfloat16)
    rest = (proj - high.astype(jnp.float32)).astype(jnp.bfloat16)
    both = jnp.concatenate([high, rest], axis=0)
    wait_for(c_v.at[:, pl.ds(0, (NT - 1) * DQK)], recv_sem.at[1])
    part = jnp.dot(both, c_v[...], preferred_element_type=jnp.float32)
    part = part[:32] + part[32:]
    for k in range(8):
        for t in range(NT):
            s_v[k, t] = part[4 * k : 4 * k + 4, DQK * t : DQK * (t + 1)]

    own = jnp.logical_and(lax.rem(z, 2) == c, lax.rem(z + x, NY) == y)

    def send_part(j):
        k = lax.rem(z // 2 + far_first(j // NT, 8), 8)
        to_z = 2 * k + c
        to_y = lax.rem(to_z + x, NY)
        t = lax.rem(s + 1 + lax.rem(j, NT), NT)
        here = jnp.logical_and(jnp.logical_and(to_z == z, to_y == y), t == s)

        @pl.when(here)
        def _():
            pltpu.make_async_copy(s_v.at[k, t], r_v.at[f], recv_sem.at[2]).start()

        @pl.when(jnp.logical_not(here))
        def _():
            remote(s_v.at[k, t], r_v.at[f], 2, (to_z, to_y, t // NC, lax.rem(t, NC))).start()

    each(NF, send_part)
    wait_for(r_v, recv_sem.at[2])

    low = jnp.sum(r_v[...], axis=0)
    update = moments(first_v[...], second_v[...], low)[2]
    u_v[f] = update
    t_v[s] = jnp.sum(update * update, axis=0, keepdims=True)
    each(NT - 1, lambda j: remote(t_v.at[s], t_v.at[s], 3, tp_peer(j)).start())
    each(NF - 1, lambda j: remote(u_v.at[f], u_v.at[f], 4, fs_peer(j)).start())
    wait_for(t_v.at[pl.ds(0, NT - 1)], recv_sem.at[3])
    g_v[f] = jnp.sum(t_v[...], axis=0)
    each(NF - 1, lambda j: remote(g_v.at[f], g_v.at[f], 5, fs_peer(j)).start())
    wait_for(u_v.at[pl.ds(0, NF - 1)], recv_sem.at[4])

    whole = u_v[...].reshape(RANK, DQK)
    head_mean = jnp.sum(whole * whole) / (RANK * DQK)
    high = whole.astype(jnp.bfloat16)
    rest = whole - high.astype(jnp.float32)
    middle = rest.astype(jnp.bfloat16)
    least = (rest - middle.astype(jnp.float32)).astype(jnp.bfloat16)
    basis = b_v[...]
    raw = (jnp.dot(basis, high, preferred_element_type=jnp.float32)
           + (jnp.dot(basis, middle, preferred_element_type=jnp.float32)
              + jnp.dot(basis, least, preferred_element_type=jnp.float32)))
    wait_for(g_v.at[pl.ds(0, NF - 1)], recv_sem.at[5])
    whole_mean = jnp.sum(g_v[...]) / (RANK * HEADS * DQK)
    out_ref[0:32] = raw
    out_ref[32:36] = low
    out_ref[36:40] = jnp.full((4, DQK), head_mean + whole_mean, jnp.float32)

    wait_for(p_v.at[pl.ds(0, NF - 1)], send_sem.at[0])
    wait_for(c_v.at[:, pl.ds(0, (NT - 1) * DQK)], send_sem.at[1])

    @pl.when(own)
    def _():
        wait_for(r_v.at[pl.ds(0, NF - 1)], send_sem.at[2])

    @pl.when(jnp.logical_not(own))
    def _():
        wait_for(r_v, send_sem.at[2])

    wait_for(t_v.at[pl.ds(0, NT - 1)], send_sem.at[3])
    wait_for(u_v.at[pl.ds(0, NF - 1)], send_sem.at[4])
    wait_for(g_v.at[pl.ds(0, NF - 1)], send_sem.at[5])


def body(inputs, query_cot, query_basis, query_master, query_first, query_second):
    bf16, f32 = jnp.bfloat16, jnp.float32
    out = pl.pallas_call(
        kernel,
        out_shape=jax.ShapeDtypeStruct((40, DQK), f32),
        in_specs=[pl.BlockSpec(memory_space=pl.ANY)] * 5,
        out_specs=pl.BlockSpec(memory_space=pltpu.VMEM),
        scratch_shapes=[
            pltpu.VMEM((256, 2048), bf16),
            pltpu.VMEM((256, NT * DQK), bf16),
            pltpu.VMEM((32, RANK), bf16),
            pltpu.VMEM((4, DQK), f32),
            pltpu.VMEM((4, DQK), f32),
            pltpu.VMEM((NF, 8, 128), bf16),
            pltpu.VMEM((8, NT, 4, DQK), f32),
            pltpu.VMEM((NF, 4, DQK), f32),
            pltpu.VMEM((NF, 4, DQK), f32),
            pltpu.VMEM((NT, 1, DQK), f32),
            pltpu.VMEM((NF, 1, DQK), f32),
            pltpu.SemaphoreType.DMA((5,)),
            pltpu.SemaphoreType.DMA((6,)),
            pltpu.SemaphoreType.DMA((6,)),
        ],
        compiler_params=pltpu.CompilerParams(collective_id=0, has_side_effects=True),
    )(inputs, query_cot, query_basis, query_first, query_second)
    factor = 1.0 / jnp.sqrt(out[36:37])
    step_q = out[0:32] * factor
    first_q, second_q, _ = moments(query_first, query_second, out[32:36])
    copy_q = (query_master + step_q).astype(bf16)
    return (step_q, first_q, second_q, copy_q)


def solution(mesh):
    torus = Mesh(mesh.devices.reshape(NZ, NY, NX, NC), ("z", "y", "x", "c"))
    in_specs = (P(FS, None), P(FS, TP), P(FS, None), P(FS, TP), P(FS, TP), P(FS, TP))
    out_specs = (P(FS, TP), P(FS, TP), P(FS, TP), P(FS, TP))
    return jax.shard_map(body, mesh=torus, in_specs=in_specs, out_specs=out_specs, check_vma=False)
```

```python
import jax
import jax.numpy as jnp
from jax import lax
from jax.experimental import pallas as pl
from jax.experimental.pallas import tpu as pltpu
from jax.sharding import Mesh
from jax.sharding import PartitionSpec as P

HEADS = 8
DQK = 128
RANK = 256
NZ, NY, NX, NC = 16, 4, 4, 2
NF, NT = NZ * NY, NX * NC
TP = ("x", "c")
FS = ("z", "y")
MESH = pl.DeviceIdType.MESH
BASIS, UPDATE, PARTS, NEAR, LINE, CORE, CROSS = 0, 1, 2, 3, 4, 5, 6
Y_ORDER = (2, 1, 3, 0)


def moments(first, second, low_grad):
    first_new = 0.8 * first + 0.2 * low_grad
    second_new = 0.9 * second + 0.1 * low_grad * low_grad
    return (first_new, second_new, first_new / jnp.sqrt(second_new))


def kernel(x_hbm, c_hbm, b_hbm, first_hbm, second_hbm, out_ref,
           x_v, c_v, b_v, first_v, second_v, p_v, s_v, r_v, u_v, n_v, g_v,
           local_sem, send_sem, recv_sem):
    z, y, x, c = (lax.axis_index(a) for a in ("z", "y", "x", "c"))
    f, s = z * NY + y, x * NC + c
    asides = [lax.rem(y + d, NY) for d in Y_ORDER]
    places = [lax.rem(s + j, NT) for j in range(1, NT)] + [s]
    sides = [(lax.div(t, NC), lax.rem(t, NC)) for t in places]

    def to_fs(do):
        def ring(k, carry):
            h = lax.div(k + 1, 2)
            to_z = lax.rem(z + 8 + h * (1 - 2 * lax.rem(k, 2)), NZ)
            for to_y in asides:
                do((to_z, to_y, x, c))
            return carry
        lax.fori_loop(0, NZ - 1, ring, 0)
        for to_y in asides[:-1]:
            do((z, to_y, x, c))

    def to_tp(do):
        for to_x, to_c in sides[:-1]:
            do((z, y, to_x, to_c))

    def remote(src, dst, phase, peer):
        return pltpu.make_async_remote_copy(src_ref=src, dst_ref=dst, send_sem=send_sem.at[phase],
                                            recv_sem=recv_sem.at[phase], device_id=peer, device_id_type=MESH)

    def wait_for(window, sem):
        pltpu.make_async_copy(window, window, sem).wait()

    barrier = pltpu.get_barrier_semaphore()
    to_fs(lambda peer: pl.semaphore_signal(barrier, inc=1, device_id=peer, device_id_type=MESH))
    to_tp(lambda peer: pl.semaphore_signal(barrier, inc=1, device_id=peer, device_id_type=MESH))

    def columns(t):
        return c_v.at[:, pl.ds(pl.multiple_of(t * DQK, DQK), DQK)]

    loads = [pltpu.make_async_copy(src, dst, local_sem.at[i]) for i, (src, dst) in enumerate((
        (b_hbm, b_v), (c_hbm, columns(s)), (x_hbm, x_v), (first_hbm, first_v), (second_hbm, second_v)))]
    for load in loads:
        load.start()

    lane = lax.broadcasted_iota(jnp.int32, (RANK, 128), 1)
    row = lax.broadcasted_iota(jnp.int32, (RANK, 128), 0)
    slot = lane & 31
    to_z = 2 * (slot >> 2) + c
    chosen = row == 16 * to_z + 4 * ((to_z + x) & 3) + (slot & 3)
    select = jnp.where(chosen, 1.0, 0.0).astype(jnp.bfloat16)
    group = lax.broadcasted_iota(jnp.int32, (8, 128), 1) >> 5
    loads[0].wait()
    picked = jnp.dot(b_v[...], select, preferred_element_type=jnp.float32)
    packed = jnp.zeros((8, 128), jnp.float32)
    for j in range(4):
        packed = jnp.where(group == j, picked[8 * j : 8 * j + 8], packed)
    p_v[f] = packed.astype(jnp.bfloat16)
    for load in loads[1:]:
        load.wait()

    pl.semaphore_wait(barrier, NF - 1 + NT - 1)
    across = [lax.rem(x + d, NX) for d in (2, 1, 3)]
    partner = (z, y, x, 1 - c)
    for i, to_x in enumerate(across):
        remote(columns(s), columns(s), CROSS + i, (z, y, to_x, c)).start()
    remote(columns(s), columns(s), CORE, partner).start()
    to_fs(lambda peer: remote(p_v.at[f], p_v.at[f], BASIS, peer).start())
    for i in (1, 2, 0):
        came = columns(lax.rem(x + NX - (2, 1, 3)[i], NX) * NC + c)
        wait_for(came, recv_sem.at[CROSS + i])
        remote(came, came, CORE, partner).start()
    wait_for(p_v.at[pl.ds(0, NF - 1)], recv_sem.at[BASIS])

    blocks = p_v[...].astype(jnp.float32)
    which = lax.broadcasted_iota(jnp.int32, (NF, 4, 8, 128), 1)
    lanes = lax.broadcasted_iota(jnp.int32, (NF, 4, 8, 128), 3) >> 5
    spread = jnp.where(which == lanes, blocks[:, None], 0.0).reshape(NF * 32, 128).astype(jnp.bfloat16)
    wide = jnp.dot(x_v[...], spread, preferred_element_type=jnp.float32).T
    proj = wide[0:32] + wide[32:64] + wide[64:96] + wide[96:128]
    high = proj.astype(jnp.bfloat16)
    rest = (proj - high.astype(jnp.float32)).astype(jnp.bfloat16)
    both = jnp.concatenate([high, rest], axis=0)
    wait_for(c_v.at[:, pl.ds(0, NX * DQK)], recv_sem.at[CORE])
    part = jnp.dot(both, c_v[...], preferred_element_type=jnp.float32)
    part = part[:32] + part[32:]
    for k in range(8):
        for t in range(NT):
            s_v[k, t] = part[4 * k : 4 * k + 4, DQK * t : DQK * (t + 1)]

    own = jnp.logical_and(lax.rem(z, 2) == c, lax.rem(z + x, NY) == y)

    def send_parts(j, carry):
        h = lax.div(j + 1, 2)
        k = lax.rem(lax.div(z, 2) + 4 + h * (1 - 2 * lax.rem(j, 2)), 8)
        to_z = 2 * k + c
        to_y = lax.rem(to_z + x, NY)
        for t, (to_x, to_c) in zip(places[:-1], sides):
            remote(s_v.at[k, t], r_v.at[f], PARTS, (to_z, to_y, to_x, to_c)).start()
        here = jnp.logical_and(to_z == z, to_y == y)

        @pl.when(here)
        def _():
            pltpu.make_async_copy(s_v.at[k, s], r_v.at[f], recv_sem.at[PARTS]).start()

        @pl.when(jnp.logical_not(here))
        def _():
            remote(s_v.at[k, s], r_v.at[f], PARTS, (to_z, to_y, x, c)).start()

        return carry

    lax.fori_loop(0, 8, send_parts, 0)
    wait_for(r_v, recv_sem.at[PARTS])

    low = jnp.sum(r_v[...], axis=0)
    update = moments(first_v[...], second_v[...], low)[2]
    spot = y * NT + s
    n_v[spot] = jnp.sum(update * update, axis=0, keepdims=True)
    u_v[f] = update
    for to_y in asides:
        for to_x, to_c in (sides[:-1] if to_y is asides[-1] else sides):
            remote(n_v.at[spot], n_v.at[spot], NEAR, (z, to_y, to_x, to_c)).start()

    def others(do):
        def ring(k, carry):
            do(jnp.where(k >= z, k + 1, k))
            return carry
        lax.fori_loop(0, NZ - 1, ring, 0)

    def send_update(to_z):
        for to_y in asides:
            remote(u_v.at[f], u_v.at[f], UPDATE, (to_z, to_y, x, c)).start()

    others(send_update)
    for to_y in asides[:-1]:
        remote(u_v.at[f], u_v.at[f], UPDATE, (z, to_y, x, c)).start()
    out_ref[32:36] = low
    wait_for(n_v.at[pl.ds(0, NY * NT - 1)], recv_sem.at[NEAR])
    g_v[z] = jnp.sum(n_v[...], axis=0)
    others(lambda to_z: remote(g_v.at[z], g_v.at[z], LINE, (to_z, y, x, c)).start())
    wait_for(u_v.at[pl.ds(0, NF - 1)], recv_sem.at[UPDATE])

    whole = u_v[...].reshape(RANK, DQK)
    high = whole.astype(jnp.bfloat16)
    rest = whole - high.astype(jnp.float32)
    middle = rest.astype(jnp.bfloat16)
    least = (rest - middle.astype(jnp.float32)).astype(jnp.bfloat16)
    basis = b_v[...]
    out_ref[0:32] = (jnp.dot(basis, high, preferred_element_type=jnp.float32)
                     + (jnp.dot(basis, middle, preferred_element_type=jnp.float32)
                        + jnp.dot(basis, least, preferred_element_type=jnp.float32)))
    head_mean = jnp.sum(whole * whole) / (RANK * DQK)

    wait_for(p_v.at[pl.ds(0, NF - 1)], send_sem.at[BASIS])
    for i in range(3):
        wait_for(columns(0), send_sem.at[CROSS + i])
    wait_for(c_v.at[:, pl.ds(0, NX * DQK)], send_sem.at[CORE])

    @pl.when(own)
    def _():
        wait_for(r_v.at[pl.ds(0, NF - 1)], send_sem.at[PARTS])

    @pl.when(jnp.logical_not(own))
    def _():
        wait_for(r_v, send_sem.at[PARTS])

    wait_for(u_v.at[pl.ds(0, NF - 1)], send_sem.at[UPDATE])
    wait_for(n_v.at[pl.ds(0, NY * NT - 1)], send_sem.at[NEAR])
    wait_for(g_v.at[pl.ds(0, NZ - 1)], recv_sem.at[LINE])
    whole_mean = jnp.sum(g_v[...]) / (RANK * HEADS * DQK)
    out_ref[36:40] = jnp.full((4, DQK), head_mean + whole_mean, jnp.float32)
    wait_for(g_v.at[pl.ds(0, NZ - 1)], send_sem.at[LINE])


def finish(sums_ref, master_ref, first_ref, second_ref, step_ref, first_out, second_out, copy_ref):
    factor = 1.0 / jnp.sqrt(sums_ref[36:37])
    step = sums_ref[0:32] * factor
    step_ref[...] = step
    copy_ref[...] = (master_ref[...] + step).astype(jnp.bfloat16)
    first_out[...], second_out[...], _ = moments(first_ref[...], second_ref[...], sums_ref[32:36])


def body(inputs, query_cot, query_basis, query_master, query_first, query_second):
    bf16, f32 = jnp.bfloat16, jnp.float32
    sums = pl.pallas_call(
        kernel,
        out_shape=pltpu.VMEM((40, DQK), f32),
        in_specs=[pl.BlockSpec(memory_space=pl.ANY)] * 5,
        out_specs=pl.BlockSpec(memory_space=pltpu.VMEM),
        scratch_shapes=[
            pltpu.VMEM((256, 2048), bf16),
            pltpu.VMEM((256, NT * DQK), bf16),
            pltpu.VMEM((32, RANK), bf16),
            pltpu.VMEM((4, DQK), f32),
            pltpu.VMEM((4, DQK), f32),
            pltpu.VMEM((NF, 8, 128), bf16),
            pltpu.VMEM((8, NT, 4, DQK), f32),
            pltpu.VMEM((NF, 4, DQK), f32),
            pltpu.VMEM((NF, 4, DQK), f32),
            pltpu.VMEM((NY * NT, 1, DQK), f32),
            pltpu.VMEM((NZ, 1, DQK), f32),
            pltpu.SemaphoreType.DMA((5,)),
            pltpu.SemaphoreType.DMA((9,)),
            pltpu.SemaphoreType.DMA((9,)),
        ],
        compiler_params=pltpu.CompilerParams(collective_id=0, has_side_effects=True),
    )(inputs, query_cot, query_basis, query_first, query_second)
    vmem = pl.BlockSpec(memory_space=pltpu.VMEM)
    in_vmem = lambda a: pltpu.with_memory_space_constraint(a, pltpu.VMEM)
    return pl.pallas_call(
        finish,
        out_shape=(jax.ShapeDtypeStruct((32, DQK), f32), jax.ShapeDtypeStruct((4, DQK), f32),
                   jax.ShapeDtypeStruct((4, DQK), f32), jax.ShapeDtypeStruct((32, DQK), bf16)),
        in_specs=[vmem] * 4,
        out_specs=(vmem,) * 4,
    )(in_vmem(sums), in_vmem(query_master), in_vmem(query_first), in_vmem(query_second))


def solution(mesh):
    torus = Mesh(mesh.devices.reshape(NZ, NY, NX, NC), ("z", "y", "x", "c"))
    in_specs = (P(FS, None), P(FS, TP), P(FS, None), P(FS, TP), P(FS, TP), P(FS, TP))
    out_specs = (P(FS, TP), P(FS, TP), P(FS, TP), P(FS, TP))
    return jax.shard_map(body, mesh=torus, in_specs=in_specs, out_specs=out_specs, check_vma=False)
```

```python
import jax
import jax.numpy as jnp
from jax import lax
from jax.experimental import pallas as pl
from jax.experimental.pallas import tpu as pltpu
from jax.sharding import Mesh
from jax.sharding import PartitionSpec as P

HEADS = 8
DQK = 128
RANK = 256
NZ, NY, NX, NC = 16, 4, 4, 2
NF, NT = NZ * NY, NX * NC
TP = ("x", "c")
FS = ("z", "y")
MESH = pl.DeviceIdType.MESH
BASIS, UPDATE, PARTS, NEAR, LINE, MOMENTS, LOW, CORE, CROSS = 0, 1, 2, 3, 4, 5, 6, 7, 8
Y_ORDER = (2, 1, 3, 0)


def moments(first, second, low_grad):
    first_new = 0.8 * first + 0.2 * low_grad
    second_new = 0.9 * second + 0.1 * low_grad * low_grad
    return (first_new, second_new, first_new / jnp.sqrt(second_new))


def kernel(x_hbm, c_hbm, b_hbm, first_hbm, second_hbm, out_ref,
           x_v, c_v, b_v, own_v, for_v, new_v, p_v, s_v, r_v, u_v, n_v, g_v, l_v,
           local_sem, send_sem, recv_sem):
    z, y, x, c = (lax.axis_index(a) for a in ("z", "y", "x", "c"))
    f, s = z * NY + y, x * NC + c
    asides = [lax.rem(y + d, NY) for d in Y_ORDER]
    places = [lax.rem(s + j, NT) for j in range(1, NT)] + [s]
    sides = [(lax.div(t, NC), lax.rem(t, NC)) for t in places]

    def to_fs(do):
        def ring(k, carry):
            h = lax.div(k + 1, 2)
            to_z = lax.rem(z + 8 + h * (1 - 2 * lax.rem(k, 2)), NZ)
            for to_y in asides:
                do((to_z, to_y, x, c))
            return carry
        lax.fori_loop(0, NZ - 1, ring, 0)
        for to_y in asides[:-1]:
            do((z, to_y, x, c))

    def to_tp(do):
        for to_x, to_c in sides[:-1]:
            do((z, y, to_x, to_c))

    def remote(src, dst, phase, peer):
        return pltpu.make_async_remote_copy(src_ref=src, dst_ref=dst, send_sem=send_sem.at[phase],
                                            recv_sem=recv_sem.at[phase], device_id=peer, device_id_type=MESH)

    def wait_for(window, sem):
        pltpu.make_async_copy(window, window, sem).wait()

    barrier = pltpu.get_barrier_semaphore()
    to_fs(lambda peer: pl.semaphore_signal(barrier, inc=1, device_id=peer, device_id_type=MESH))
    to_tp(lambda peer: pl.semaphore_signal(barrier, inc=1, device_id=peer, device_id_type=MESH))

    def columns(t):
        return c_v.at[:, pl.ds(pl.multiple_of(t * DQK, DQK), DQK)]

    loads = [pltpu.make_async_copy(src, dst, local_sem.at[i]) for i, (src, dst) in enumerate((
        (b_hbm, b_v), (c_hbm, columns(s)), (x_hbm, x_v), (first_hbm, own_v.at[0]), (second_hbm, own_v.at[1])))]
    for load in loads:
        load.start()

    def block(at_z, at_y):
        turned = lax.rem(at_z + 2, NZ)
        to_x = lax.rem(x + 6 - lax.div(turned, 4), NX)
        return 2 * lax.rem(turned, 4) + lax.div(at_y, 2), to_x, lax.rem(at_y, 2)

    sum_k, sum_x, sum_c = block(z, y)
    sum_f = 8 * s + sum_k
    client = (lax.div(sum_f, NY), lax.rem(sum_f, NY), sum_x, sum_c)
    its_s, its_k = lax.div(f, 8), lax.rem(f, 8)
    its_x = lax.div(its_s, NC)
    its_turned = 4 * lax.rem(its_x + 6 - x, NX) + lax.div(its_k, 2)
    server = (lax.rem(its_turned + 14, NZ), 2 * lax.rem(its_k, 2) + c, its_x, lax.rem(its_s, NC))
    alone = jnp.logical_and(jnp.logical_and(server[0] == z, server[1] == y), its_s == s)

    lane = lax.broadcasted_iota(jnp.int32, (RANK, 128), 1)
    row = lax.broadcasted_iota(jnp.int32, (RANK, 128), 0)
    chosen = row == 32 * s + (lane & 31)
    select = jnp.where(chosen, 1.0, 0.0).astype(jnp.bfloat16)
    group = lax.broadcasted_iota(jnp.int32, (8, 128), 1) >> 5
    loads[0].wait()
    picked = jnp.dot(b_v[...], select, preferred_element_type=jnp.float32)
    packed = jnp.zeros((8, 128), jnp.float32)
    for j in range(4):
        packed = jnp.where(group == j, picked[8 * j : 8 * j + 8], packed)
    p_v[f] = packed.astype(jnp.bfloat16)
    for load in loads[1:]:
        load.wait()

    pl.semaphore_wait(barrier, NF - 1 + NT - 1)
    across = [lax.rem(x + d, NX) for d in (2, 1, 3)]
    partner = (z, y, x, 1 - c)
    for i, to_x in enumerate(across):
        remote(columns(s), columns(s), CROSS + i, (z, y, to_x, c)).start()
    remote(columns(s), columns(s), CORE, partner).start()
    to_fs(lambda peer: remote(p_v.at[f], p_v.at[f], BASIS, peer).start())
    for i in (1, 2, 0):
        came = columns(lax.rem(x + NX - (2, 1, 3)[i], NX) * NC + c)
        wait_for(came, recv_sem.at[CROSS + i])
        remote(came, came, CORE, partner).start()
    wait_for(c_v.at[:, pl.ds(0, NX * DQK)], recv_sem.at[CORE])

    @pl.when(alone)
    def _():
        pltpu.make_async_copy(own_v, for_v, recv_sem.at[MOMENTS]).start()

    @pl.when(jnp.logical_not(alone))
    def _():
        remote(own_v, for_v, MOMENTS, server).start()

    wait_for(p_v.at[pl.ds(0, NF - 1)], recv_sem.at[BASIS])

    blocks = p_v[...].astype(jnp.float32)
    which = lax.broadcasted_iota(jnp.int32, (NF, 4, 8, 128), 1)
    lanes = lax.broadcasted_iota(jnp.int32, (NF, 4, 8, 128), 3) >> 5
    spread = jnp.where(which == lanes, blocks[:, None], 0.0).reshape(NF * 32, 128).astype(jnp.bfloat16)
    wide = jnp.dot(x_v[...], spread, preferred_element_type=jnp.float32).T
    proj = wide[0:32] + wide[32:64] + wide[64:96] + wide[96:128]
    high = proj.astype(jnp.bfloat16)
    rest = (proj - high.astype(jnp.float32)).astype(jnp.bfloat16)
    both = jnp.concatenate([high, rest], axis=0)
    part = jnp.dot(both, c_v[...], preferred_element_type=jnp.float32)
    part = part[:32] + part[32:]
    for k in range(8):
        for t in range(NT):
            s_v[k, t] = part[4 * k : 4 * k + 4, DQK * t : DQK * (t + 1)]

    low_bits = [(lax.div(to_y, 2), lax.rem(to_y, 2)) for to_y in asides]

    def parts_ring(n, carry):
        h = lax.div(n + 1, 2)
        to_z = lax.rem(z + 8 + h * (1 - 2 * lax.rem(n, 2)), NZ)
        turned = lax.rem(to_z + 2, NZ)
        to_k = 2 * lax.rem(turned, 4)
        to_t = NC * lax.rem(x + 6 - lax.div(turned, 4), NX)
        for to_y, (to_half, to_c) in zip(asides, low_bits):
            remote(s_v.at[to_k + to_half, to_t + to_c], r_v.at[f], PARTS, (to_z, to_y, x, c)).start()
        return carry

    lax.fori_loop(0, NZ - 1, parts_ring, 0)
    for to_y in asides[:-1]:
        k, to_x, to_c = block(z, to_y)
        remote(s_v.at[k, to_x * NC + to_c], r_v.at[f], PARTS, (z, to_y, x, c)).start()
    pltpu.make_async_copy(s_v.at[sum_k, sum_x * NC + sum_c], r_v.at[f], recv_sem.at[PARTS]).start()
    wait_for(for_v, recv_sem.at[MOMENTS])
    wait_for(r_v, recv_sem.at[PARTS])

    low = jnp.sum(r_v[...], axis=0)
    update = moments(for_v[0], for_v[1], low)[2]
    spot = y * NT + s
    n_v[spot] = jnp.sum(update * update, axis=0, keepdims=True)
    new_v[0] = update
    new_v[1] = low
    for to_y in asides:
        for to_x, to_c in (sides[:-1] if to_y is asides[-1] else sides):
            remote(n_v.at[spot], n_v.at[spot], NEAR, (z, to_y, to_x, to_c)).start()

    def others(do):
        def ring(k, carry):
            do(jnp.where(k >= z, k + 1, k))
            return carry
        lax.fori_loop(0, NZ - 1, ring, 0)

    def send_update(to_z):
        for to_y in asides:
            remote(new_v.at[0], u_v.at[sum_f], UPDATE, (to_z, to_y, sum_x, sum_c)).start()

    others(send_update)
    for to_y in asides[:-1]:
        remote(new_v.at[0], u_v.at[sum_f], UPDATE, (z, to_y, sum_x, sum_c)).start()
    home = jnp.logical_and(sum_x == x, sum_c == c)

    @pl.when(home)
    def _():
        pltpu.make_async_copy(new_v.at[0], u_v.at[sum_f], recv_sem.at[UPDATE]).start()

    @pl.when(jnp.logical_not(home))
    def _():
        remote(new_v.at[0], u_v.at[sum_f], UPDATE, (z, y, sum_x, sum_c)).start()

    @pl.when(alone)
    def _():
        pltpu.make_async_copy(new_v.at[1], l_v, recv_sem.at[LOW]).start()

    @pl.when(jnp.logical_not(alone))
    def _():
        remote(new_v.at[1], l_v, LOW, client).start()

    wait_for(n_v.at[pl.ds(0, NY * NT - 1)], recv_sem.at[NEAR])
    g_v[z] = jnp.sum(n_v[...], axis=0)
    others(lambda to_z: remote(g_v.at[z], g_v.at[z], LINE, (to_z, y, x, c)).start())
    wait_for(u_v, recv_sem.at[UPDATE])

    whole = u_v[...].reshape(RANK, DQK)
    high = whole.astype(jnp.bfloat16)
    rest = whole - high.astype(jnp.float32)
    middle = rest.astype(jnp.bfloat16)
    least = (rest - middle.astype(jnp.float32)).astype(jnp.bfloat16)
    basis = b_v[...]
    out_ref[0:32] = (jnp.dot(basis, high, preferred_element_type=jnp.float32)
                     + (jnp.dot(basis, middle, preferred_element_type=jnp.float32)
                        + jnp.dot(basis, least, preferred_element_type=jnp.float32)))
    head_mean = jnp.sum(whole * whole) / (RANK * DQK)

    wait_for(p_v.at[pl.ds(0, NF - 1)], send_sem.at[BASIS])
    for i in range(3):
        wait_for(columns(0), send_sem.at[CROSS + i])
    wait_for(c_v.at[:, pl.ds(0, NX * DQK)], send_sem.at[CORE])

    wait_for(r_v.at[pl.ds(0, NF - 1)], send_sem.at[PARTS])

    @pl.when(home)
    def _():
        wait_for(u_v.at[pl.ds(0, NF - 1)], send_sem.at[UPDATE])

    @pl.when(jnp.logical_not(home))
    def _():
        wait_for(u_v, send_sem.at[UPDATE])

    @pl.when(jnp.logical_not(alone))
    def _():
        wait_for(own_v, send_sem.at[MOMENTS])
        wait_for(l_v, send_sem.at[LOW])

    wait_for(l_v, recv_sem.at[LOW])
    out_ref[32:36] = l_v[...]
    wait_for(n_v.at[pl.ds(0, NY * NT - 1)], send_sem.at[NEAR])
    wait_for(g_v.at[pl.ds(0, NZ - 1)], recv_sem.at[LINE])
    whole_mean = jnp.sum(g_v[...]) / (RANK * HEADS * DQK)
    out_ref[36:40] = jnp.full((4, DQK), head_mean + whole_mean, jnp.float32)
    wait_for(g_v.at[pl.ds(0, NZ - 1)], send_sem.at[LINE])


def finish(sums_ref, master_ref, first_ref, second_ref, step_ref, first_out, second_out, copy_ref):
    factor = 1.0 / jnp.sqrt(sums_ref[36:37])
    step = sums_ref[0:32] * factor
    step_ref[...] = step
    copy_ref[...] = (master_ref[...] + step).astype(jnp.bfloat16)
    first_out[...], second_out[...], _ = moments(first_ref[...], second_ref[...], sums_ref[32:36])


def body(inputs, query_cot, query_basis, query_master, query_first, query_second):
    bf16, f32 = jnp.bfloat16, jnp.float32
    sums = pl.pallas_call(
        kernel,
        out_shape=pltpu.VMEM((40, DQK), f32),
        in_specs=[pl.BlockSpec(memory_space=pl.ANY)] * 5,
        out_specs=pl.BlockSpec(memory_space=pltpu.VMEM),
        scratch_shapes=[
            pltpu.VMEM((256, 2048), bf16),
            pltpu.VMEM((256, NT * DQK), bf16),
            pltpu.VMEM((32, RANK), bf16),
            pltpu.VMEM((2, 4, DQK), f32),
            pltpu.VMEM((2, 4, DQK), f32),
            pltpu.VMEM((2, 4, DQK), f32),
            pltpu.VMEM((NF, 8, 128), bf16),
            pltpu.VMEM((8, NT, 4, DQK), f32),
            pltpu.VMEM((NF, 4, DQK), f32),
            pltpu.VMEM((NF, 4, DQK), f32),
            pltpu.VMEM((NY * NT, 1, DQK), f32),
            pltpu.VMEM((NZ, 1, DQK), f32),
            pltpu.VMEM((4, DQK), f32),
            pltpu.SemaphoreType.DMA((5,)),
            pltpu.SemaphoreType.DMA((11,)),
            pltpu.SemaphoreType.DMA((11,)),
        ],
        compiler_params=pltpu.CompilerParams(collective_id=0, has_side_effects=True),
    )(inputs, query_cot, query_basis, query_first, query_second)
    vmem = pl.BlockSpec(memory_space=pltpu.VMEM)
    in_vmem = lambda a: pltpu.with_memory_space_constraint(a, pltpu.VMEM)
    return pl.pallas_call(
        finish,
        out_shape=(jax.ShapeDtypeStruct((32, DQK), f32), jax.ShapeDtypeStruct((4, DQK), f32),
                   jax.ShapeDtypeStruct((4, DQK), f32), jax.ShapeDtypeStruct((32, DQK), bf16)),
        in_specs=[vmem] * 4,
        out_specs=(vmem,) * 4,
    )(in_vmem(sums), in_vmem(query_master), in_vmem(query_first), in_vmem(query_second))


def solution(mesh):
    torus = Mesh(mesh.devices.reshape(NZ, NY, NX, NC), ("z", "y", "x", "c"))
    in_specs = (P(FS, None), P(FS, TP), P(FS, None), P(FS, TP), P(FS, TP), P(FS, TP))
    out_specs = (P(FS, TP), P(FS, TP), P(FS, TP), P(FS, TP))
    return jax.shard_map(body, mesh=torus, in_specs=in_specs, out_specs=out_specs, check_vma=False)
```

```python
import jax
import jax.numpy as jnp
from jax import lax
from jax.experimental import pallas as pl
from jax.experimental.pallas import tpu as pltpu
from jax.sharding import Mesh
from jax.sharding import PartitionSpec as P

HEADS = 8
DQK = 128
RANK = 256
NZ, NY, NX, NC = 16, 4, 4, 2
NF, NT = NZ * NY, NX * NC
TP = ("x", "c")
FS = ("z", "y")
MESH = pl.DeviceIdType.MESH
BASIS, UPDATE, PARTS, NEAR, LINE, MOMENTS, LOW, CORE, CROSS = 0, 1, 2, 3, 4, 5, 6, 7, 8
Y_ORDER = (2, 1, 3, 0)


def moments(first, second, low_grad):
    first_new = 0.8 * first + 0.2 * low_grad
    second_new = 0.9 * second + 0.1 * low_grad * low_grad
    return (first_new, second_new, first_new / jnp.sqrt(second_new))


def kernel(x_hbm, c_hbm, b_hbm, first_hbm, second_hbm, out_ref,
           x_v, c_v, b_v, own_v, for_v, new_v, p_v, s_v, r_v, u_v, n_v, g_v, l_v,
           local_sem, send_sem, recv_sem):
    z, y, x, c = (lax.axis_index(a) for a in ("z", "y", "x", "c"))
    f, s = z * NY + y, x * NC + c
    asides = [lax.rem(y + d, NY) for d in Y_ORDER]
    places = [lax.rem(s + j, NT) for j in range(1, NT)] + [s]
    sides = [(lax.div(t, NC), lax.rem(t, NC)) for t in places]

    def to_fs(do):
        def ring(k, carry):
            h = lax.div(k + 1, 2)
            to_z = lax.rem(z + 8 + h * (1 - 2 * lax.rem(k, 2)), NZ)
            for to_y in asides:
                do((to_z, to_y, x, c))
            return carry
        lax.fori_loop(0, NZ - 1, ring, 0)
        for to_y in asides[:-1]:
            do((z, to_y, x, c))

    def to_tp(do):
        for to_x, to_c in sides[:-1]:
            do((z, y, to_x, to_c))

    def remote(src, dst, phase, peer):
        return pltpu.make_async_remote_copy(src_ref=src, dst_ref=dst, send_sem=send_sem.at[phase],
                                            recv_sem=recv_sem.at[phase], device_id=peer, device_id_type=MESH)

    def wait_for(window, sem):
        pltpu.make_async_copy(window, window, sem).wait()

    barrier = pltpu.get_barrier_semaphore()
    to_fs(lambda peer: pl.semaphore_signal(barrier, inc=1, device_id=peer, device_id_type=MESH))
    to_tp(lambda peer: pl.semaphore_signal(barrier, inc=1, device_id=peer, device_id_type=MESH))

    def columns(t):
        return c_v.at[:, pl.ds(pl.multiple_of(t * DQK, DQK), DQK)]

    loads = [pltpu.make_async_copy(src, dst, local_sem.at[i]) for i, (src, dst) in enumerate((
        (b_hbm, b_v), (c_hbm, columns(s)), (x_hbm, x_v), (first_hbm, own_v.at[0]), (second_hbm, own_v.at[1])))]
    for load in loads:
        load.start()

    def block(at_z, at_y):
        turned = lax.rem(at_z + 2, NZ)
        to_x = lax.rem(x + 6 - lax.div(turned, 4), NX)
        return 2 * lax.rem(turned, 4) + lax.div(at_y, 2), to_x, lax.rem(at_y, 2)

    sum_k, sum_x, sum_c = block(z, y)
    sum_f = 8 * s + sum_k
    client = (lax.div(sum_f, NY), lax.rem(sum_f, NY), sum_x, sum_c)
    its_s, its_k = lax.div(f, 8), lax.rem(f, 8)
    its_x = lax.div(its_s, NC)
    its_turned = 4 * lax.rem(its_x + 6 - x, NX) + lax.div(its_k, 2)
    server = (lax.rem(its_turned + 14, NZ), 2 * lax.rem(its_k, 2) + c, its_x, lax.rem(its_s, NC))
    alone = jnp.logical_and(jnp.logical_and(server[0] == z, server[1] == y), its_s == s)

    lane = lax.broadcasted_iota(jnp.int32, (RANK, 128), 1)
    row = lax.broadcasted_iota(jnp.int32, (RANK, 128), 0)
    chosen = row == 32 * s + (lane & 31)
    select = jnp.where(chosen, 1.0, 0.0).astype(jnp.bfloat16)
    group = lax.broadcasted_iota(jnp.int32, (8, 128), 1) >> 5
    loads[0].wait()
    picked = jnp.dot(b_v[...], select, preferred_element_type=jnp.float32)
    packed = jnp.zeros((8, 128), jnp.float32)
    for j in range(4):
        packed = jnp.where(group == j, picked[8 * j : 8 * j + 8], packed)
    p_v[f] = packed.astype(jnp.bfloat16)
    for load in loads[1:]:
        load.wait()

    pl.semaphore_wait(barrier, NF - 1 + NT - 1)
    across = [lax.rem(x + d, NX) for d in (2, 1, 3)]
    partner = (z, y, x, 1 - c)
    for i, to_x in enumerate(across):
        remote(columns(s), columns(s), CROSS + i, (z, y, to_x, c)).start()
    remote(columns(s), columns(s), CORE, partner).start()
    to_fs(lambda peer: remote(p_v.at[f], p_v.at[f], BASIS, peer).start())
    for i in (1, 2, 0):
        came = columns(lax.rem(x + NX - (2, 1, 3)[i], NX) * NC + c)
        wait_for(came, recv_sem.at[CROSS + i])
        remote(came, came, CORE, partner).start()
    wait_for(c_v.at[:, pl.ds(0, NX * DQK)], recv_sem.at[CORE])

    @pl.when(alone)
    def _():
        pltpu.make_async_copy(own_v, for_v, recv_sem.at[MOMENTS]).start()

    @pl.when(jnp.logical_not(alone))
    def _():
        remote(own_v, for_v, MOMENTS, server).start()

    wait_for(p_v.at[pl.ds(0, NF - 1)], recv_sem.at[BASIS])

    blocks = p_v[...].astype(jnp.float32)
    which = lax.broadcasted_iota(jnp.int32, (NF, 4, 8, 128), 1)
    lanes = lax.broadcasted_iota(jnp.int32, (NF, 4, 8, 128), 3) >> 5
    spread = jnp.where(which == lanes, blocks[:, None], 0.0).reshape(NF * 32, 128).astype(jnp.bfloat16)
    wide = jnp.dot(x_v[...], spread, preferred_element_type=jnp.float32).T
    proj = wide[0:32] + wide[32:64] + wide[64:96] + wide[96:128]
    high = proj.astype(jnp.bfloat16)
    rest = (proj - high.astype(jnp.float32)).astype(jnp.bfloat16)
    both = jnp.concatenate([high, rest], axis=0)
    part = jnp.dot(both, c_v[...], preferred_element_type=jnp.float32)
    part = part[:32] + part[32:]
    for k in range(8):
        for t in range(NT):
            s_v[k, t] = part[4 * k : 4 * k + 4, DQK * t : DQK * (t + 1)]

    low_bits = [(lax.div(to_y, 2), lax.rem(to_y, 2)) for to_y in asides]

    def parts_ring(n, carry):
        h = lax.div(n + 1, 2)
        to_z = lax.rem(z + 8 + h * (1 - 2 * lax.rem(n, 2)), NZ)
        turned = lax.rem(to_z + 2, NZ)
        to_k = 2 * lax.rem(turned, 4)
        to_t = NC * lax.rem(x + 6 - lax.div(turned, 4), NX)
        for to_y, (to_half, to_c) in zip(asides, low_bits):
            remote(s_v.at[to_k + to_half, to_t + to_c], r_v.at[f], PARTS, (to_z, to_y, x, c)).start()
        return carry

    lax.fori_loop(0, NZ - 1, parts_ring, 0)
    for to_y in asides[:-1]:
        k, to_x, to_c = block(z, to_y)
        remote(s_v.at[k, to_x * NC + to_c], r_v.at[f], PARTS, (z, to_y, x, c)).start()
    pltpu.make_async_copy(s_v.at[sum_k, sum_x * NC + sum_c], r_v.at[f], recv_sem.at[PARTS]).start()
    wait_for(for_v, recv_sem.at[MOMENTS])
    wait_for(r_v, recv_sem.at[PARTS])

    low = jnp.sum(r_v[...], axis=0)
    update = moments(for_v[0], for_v[1], low)[2]
    spot = s
    n_v[spot] = jnp.sum(update * update, axis=0, keepdims=True)
    new_v[0] = update
    new_v[1] = low
    to_tp(lambda peer: remote(n_v.at[spot], n_v.at[spot], NEAR, peer).start())

    def others(do):
        def ring(k, carry):
            do(jnp.where(k >= z, k + 1, k))
            return carry
        lax.fori_loop(0, NZ - 1, ring, 0)

    def send_update(to_z):
        for to_y in asides:
            remote(new_v.at[0], u_v.at[sum_f], UPDATE, (to_z, to_y, sum_x, sum_c)).start()

    others(send_update)
    for to_y in asides[:-1]:
        remote(new_v.at[0], u_v.at[sum_f], UPDATE, (z, to_y, sum_x, sum_c)).start()
    home = jnp.logical_and(sum_x == x, sum_c == c)

    @pl.when(home)
    def _():
        pltpu.make_async_copy(new_v.at[0], u_v.at[sum_f], recv_sem.at[UPDATE]).start()

    @pl.when(jnp.logical_not(home))
    def _():
        remote(new_v.at[0], u_v.at[sum_f], UPDATE, (z, y, sum_x, sum_c)).start()

    @pl.when(alone)
    def _():
        pltpu.make_async_copy(new_v.at[1], l_v, recv_sem.at[LOW]).start()

    @pl.when(jnp.logical_not(alone))
    def _():
        remote(new_v.at[1], l_v, LOW, client).start()

    wait_for(n_v.at[pl.ds(0, NT - 1)], recv_sem.at[NEAR])
    g_v[f] = jnp.sum(n_v[...], axis=0)

    def send_sum(to_z):
        for to_y in asides:
            remote(g_v.at[f], g_v.at[f], LINE, (to_z, to_y, x, c)).start()

    others(send_sum)
    for to_y in asides[:-1]:
        remote(g_v.at[f], g_v.at[f], LINE, (z, to_y, x, c)).start()
    wait_for(u_v, recv_sem.at[UPDATE])

    whole = u_v[...].reshape(RANK, DQK)
    high = whole.astype(jnp.bfloat16)
    rest = whole - high.astype(jnp.float32)
    middle = rest.astype(jnp.bfloat16)
    least = (rest - middle.astype(jnp.float32)).astype(jnp.bfloat16)
    basis = b_v[...]
    out_ref[0:32] = (jnp.dot(basis, high, preferred_element_type=jnp.float32)
                     + (jnp.dot(basis, middle, preferred_element_type=jnp.float32)
                        + jnp.dot(basis, least, preferred_element_type=jnp.float32)))
    head_mean = jnp.sum(whole * whole) / (RANK * DQK)

    wait_for(p_v.at[pl.ds(0, NF - 1)], send_sem.at[BASIS])
    for i in range(3):
        wait_for(columns(0), send_sem.at[CROSS + i])
    wait_for(c_v.at[:, pl.ds(0, NX * DQK)], send_sem.at[CORE])

    wait_for(r_v.at[pl.ds(0, NF - 1)], send_sem.at[PARTS])

    @pl.when(home)
    def _():
        wait_for(u_v.at[pl.ds(0, NF - 1)], send_sem.at[UPDATE])

    @pl.when(jnp.logical_not(home))
    def _():
        wait_for(u_v, send_sem.at[UPDATE])

    @pl.when(jnp.logical_not(alone))
    def _():
        wait_for(own_v, send_sem.at[MOMENTS])
        wait_for(l_v, send_sem.at[LOW])

    wait_for(l_v, recv_sem.at[LOW])
    out_ref[32:36] = l_v[...]
    wait_for(n_v.at[pl.ds(0, NT - 1)], send_sem.at[NEAR])
    wait_for(g_v.at[pl.ds(0, NF - 1)], recv_sem.at[LINE])
    whole_mean = jnp.sum(g_v[...]) / (RANK * HEADS * DQK)
    out_ref[36:40] = jnp.full((4, DQK), head_mean + whole_mean, jnp.float32)
    wait_for(g_v.at[pl.ds(0, NF - 1)], send_sem.at[LINE])


def finish(sums_ref, master_ref, first_ref, second_ref, step_ref, first_out, second_out, copy_ref):
    factor = 1.0 / jnp.sqrt(sums_ref[36:37])
    step = sums_ref[0:32] * factor
    step_ref[...] = step
    copy_ref[...] = (master_ref[...] + step).astype(jnp.bfloat16)
    first_out[...], second_out[...], _ = moments(first_ref[...], second_ref[...], sums_ref[32:36])


def body(inputs, query_cot, query_basis, query_master, query_first, query_second):
    bf16, f32 = jnp.bfloat16, jnp.float32
    sums = pl.pallas_call(
        kernel,
        out_shape=pltpu.VMEM((40, DQK), f32),
        in_specs=[pl.BlockSpec(memory_space=pl.ANY)] * 5,
        out_specs=pl.BlockSpec(memory_space=pltpu.VMEM),
        scratch_shapes=[
            pltpu.VMEM((256, 2048), bf16),
            pltpu.VMEM((256, NT * DQK), bf16),
            pltpu.VMEM((32, RANK), bf16),
            pltpu.VMEM((2, 4, DQK), f32),
            pltpu.VMEM((2, 4, DQK), f32),
            pltpu.VMEM((2, 4, DQK), f32),
            pltpu.VMEM((NF, 8, 128), bf16),
            pltpu.VMEM((8, NT, 4, DQK), f32),
            pltpu.VMEM((NF, 4, DQK), f32),
            pltpu.VMEM((NF, 4, DQK), f32),
            pltpu.VMEM((NT, 1, DQK), f32),
            pltpu.VMEM((NF, 1, DQK), f32),
            pltpu.VMEM((4, DQK), f32),
            pltpu.SemaphoreType.DMA((5,)),
            pltpu.SemaphoreType.DMA((11,)),
            pltpu.SemaphoreType.DMA((11,)),
        ],
        compiler_params=pltpu.CompilerParams(collective_id=0, has_side_effects=True),
    )(inputs, query_cot, query_basis, query_first, query_second)
    vmem = pl.BlockSpec(memory_space=pltpu.VMEM)
    in_vmem = lambda a: pltpu.with_memory_space_constraint(a, pltpu.VMEM)
    return pl.pallas_call(
        finish,
        out_shape=(jax.ShapeDtypeStruct((32, DQK), f32), jax.ShapeDtypeStruct((4, DQK), f32),
                   jax.ShapeDtypeStruct((4, DQK), f32), jax.ShapeDtypeStruct((32, DQK), bf16)),
        in_specs=[vmem] * 4,
        out_specs=(vmem,) * 4,
    )(in_vmem(sums), in_vmem(query_master), in_vmem(query_first), in_vmem(query_second))


def solution(mesh):
    torus = Mesh(mesh.devices.reshape(NZ, NY, NX, NC), ("z", "y", "x", "c"))
    in_specs = (P(FS, None), P(FS, TP), P(FS, None), P(FS, TP), P(FS, TP), P(FS, TP))
    out_specs = (P(FS, TP), P(FS, TP), P(FS, TP), P(FS, TP))
    return jax.shard_map(body, mesh=torus, in_specs=in_specs, out_specs=out_specs, check_vma=False)
```

```python
import jax
import jax.numpy as jnp
from jax import lax
from jax.experimental import pallas as pl
from jax.experimental.pallas import tpu as pltpu
from jax.sharding import Mesh
from jax.sharding import PartitionSpec as P

HEADS = 8
DQK = 128
RANK = 256
NZ, NY, NX, NC = 16, 4, 4, 2
NF, NT = NZ * NY, NX * NC
TP = ("x", "c")
FS = ("z", "y")
MESH = pl.DeviceIdType.MESH
BASIS, UPDATE, PARTS, NEAR, LINE, MOMENTS, LOW, CORE, CROSS = 0, 1, 2, 3, 4, 5, 6, 7, 8
Y_ORDER = (2, 1, 3, 0)


def moments(first, second, low_grad):
    first_new = 0.8 * first + 0.2 * low_grad
    second_new = 0.9 * second + 0.1 * low_grad * low_grad
    return (first_new, second_new, first_new / jnp.sqrt(second_new))


def kernel(x_hbm, c_hbm, b_hbm, first_hbm, second_hbm, out_ref,
           x_v, c_v, b_v, own_v, for_v, new_v, p_v, s_v, r_v, u_v, n_v, g_v, l_v,
           local_sem, send_sem, recv_sem):
    z, y, x, c = (lax.axis_index(a) for a in ("z", "y", "x", "c"))
    f, s = z * NY + y, x * NC + c
    asides = [lax.rem(y + d, NY) for d in Y_ORDER]
    places = [lax.rem(s + j, NT) for j in range(1, NT)] + [s]
    sides = [(lax.div(t, NC), lax.rem(t, NC)) for t in places]

    def to_fs(do):
        def ring(k, carry):
            h = lax.div(k + 1, 2)
            to_z = lax.rem(z + 8 + h * (1 - 2 * lax.rem(k, 2)), NZ)
            for to_y in asides:
                do((to_z, to_y, x, c))
            return carry
        lax.fori_loop(0, NZ - 1, ring, 0)
        for to_y in asides[:-1]:
            do((z, to_y, x, c))

    def to_tp(do):
        for to_x, to_c in sides[:-1]:
            do((z, y, to_x, to_c))

    def remote(src, dst, phase, peer):
        return pltpu.make_async_remote_copy(src_ref=src, dst_ref=dst, send_sem=send_sem.at[phase],
                                            recv_sem=recv_sem.at[phase], device_id=peer, device_id_type=MESH)

    def wait_for(window, sem):
        pltpu.make_async_copy(window, window, sem).wait()

    barrier = pltpu.get_barrier_semaphore()
    to_fs(lambda peer: pl.semaphore_signal(barrier, inc=1, device_id=peer, device_id_type=MESH))
    to_tp(lambda peer: pl.semaphore_signal(barrier, inc=1, device_id=peer, device_id_type=MESH))

    def columns(t):
        return c_v.at[:, pl.ds(pl.multiple_of(t * DQK, DQK), DQK)]

    loads = [pltpu.make_async_copy(src, dst, local_sem.at[i]) for i, (src, dst) in enumerate((
        (b_hbm, b_v), (c_hbm, columns(s)), (x_hbm, x_v), (first_hbm, own_v.at[0]), (second_hbm, own_v.at[1])))]
    for load in loads:
        load.start()

    def block(at_z, at_y):
        turned = lax.rem(at_z + 2, NZ)
        to_x = lax.rem(x + 6 - lax.div(turned, 4), NX)
        return 2 * lax.rem(turned, 4) + lax.div(at_y, 2), to_x, lax.rem(at_y, 2)

    sum_k, sum_x, sum_c = block(z, y)
    sum_f = 8 * s + sum_k
    client = (lax.div(sum_f, NY), lax.rem(sum_f, NY), sum_x, sum_c)
    its_s, its_k = lax.div(f, 8), lax.rem(f, 8)
    its_x = lax.div(its_s, NC)
    its_turned = 4 * lax.rem(its_x + 6 - x, NX) + lax.div(its_k, 2)
    server = (lax.rem(its_turned + 14, NZ), 2 * lax.rem(its_k, 2) + c, its_x, lax.rem(its_s, NC))
    alone = jnp.logical_and(jnp.logical_and(server[0] == z, server[1] == y), its_s == s)

    lane = lax.broadcasted_iota(jnp.int32, (RANK, 128), 1)
    row = lax.broadcasted_iota(jnp.int32, (RANK, 128), 0)
    chosen = row == 32 * s + (lane & 31)
    select = jnp.where(chosen, 1.0, 0.0).astype(jnp.bfloat16)
    group = lax.broadcasted_iota(jnp.int32, (8, 128), 1) >> 5
    loads[0].wait()
    picked = jnp.dot(b_v[...], select, preferred_element_type=jnp.float32)
    packed = jnp.zeros((8, 128), jnp.float32)
    for j in range(4):
        packed = jnp.where(group == j, picked[8 * j : 8 * j + 8], packed)
    p_v[f] = packed.astype(jnp.bfloat16)
    for load in loads[1:]:
        load.wait()

    pl.semaphore_wait(barrier, NF - 1 + NT - 1)
    across = [lax.rem(x + d, NX) for d in (2, 1, 3)]
    partner = (z, y, x, 1 - c)
    for i, to_x in enumerate(across):
        remote(columns(s), columns(s), CROSS + i, (z, y, to_x, c)).start()
    remote(columns(s), columns(s), CORE, partner).start()
    to_fs(lambda peer: remote(p_v.at[f], p_v.at[f], BASIS, peer).start())
    for i in (1, 2, 0):
        came = columns(lax.rem(x + NX - (2, 1, 3)[i], NX) * NC + c)
        wait_for(came, recv_sem.at[CROSS + i])
        remote(came, came, CORE, partner).start()
    wait_for(c_v.at[:, pl.ds(0, NX * DQK)], recv_sem.at[CORE])

    @pl.when(alone)
    def _():
        pltpu.make_async_copy(own_v, for_v, recv_sem.at[MOMENTS]).start()

    @pl.when(jnp.logical_not(alone))
    def _():
        remote(own_v, for_v, MOMENTS, server).start()

    wait_for(p_v.at[pl.ds(0, NF - 1)], recv_sem.at[BASIS])

    blocks = p_v[...].astype(jnp.float32)
    which = lax.broadcasted_iota(jnp.int32, (NF, 4, 8, 128), 1)
    lanes = lax.broadcasted_iota(jnp.int32, (NF, 4, 8, 128), 3) >> 5
    spread = jnp.where(which == lanes, blocks[:, None], 0.0).reshape(NF * 32, 128).astype(jnp.bfloat16)
    wide = jnp.dot(x_v[...], spread, preferred_element_type=jnp.float32).T
    proj = wide[0:32] + wide[32:64] + wide[64:96] + wide[96:128]
    high = proj.astype(jnp.bfloat16)
    rest = (proj - high.astype(jnp.float32)).astype(jnp.bfloat16)
    both = jnp.concatenate([high, rest], axis=0)
    part = jnp.dot(both, c_v[...], preferred_element_type=jnp.float32)
    part = part[:32] + part[32:]
    for k in range(8):
        for t in range(NT):
            s_v[k, t] = part[4 * k : 4 * k + 4, DQK * t : DQK * (t + 1)]

    low_bits = [(lax.div(to_y, 2), lax.rem(to_y, 2)) for to_y in asides]

    def parts_ring(n, carry):
        h = lax.div(n + 1, 2)
        to_z = lax.rem(z + 8 + h * (1 - 2 * lax.rem(n, 2)), NZ)
        turned = lax.rem(to_z + 2, NZ)
        to_k = 2 * lax.rem(turned, 4)
        to_t = NC * lax.rem(x + 6 - lax.div(turned, 4), NX)
        for to_y, (to_half, to_c) in zip(asides, low_bits):
            remote(s_v.at[to_k + to_half, to_t + to_c], r_v.at[f], PARTS, (to_z, to_y, x, c)).start()
        return carry

    lax.fori_loop(0, NZ - 1, parts_ring, 0)
    for to_y in asides[:-1]:
        k, to_x, to_c = block(z, to_y)
        remote(s_v.at[k, to_x * NC + to_c], r_v.at[f], PARTS, (z, to_y, x, c)).start()
    pltpu.make_async_copy(s_v.at[sum_k, sum_x * NC + sum_c], r_v.at[f], recv_sem.at[PARTS]).start()
    wait_for(for_v, recv_sem.at[MOMENTS])
    wait_for(r_v, recv_sem.at[PARTS])

    low = jnp.sum(r_v[...], axis=0)
    update = moments(for_v[0], for_v[1], low)[2]
    spot = y * NT + s
    n_v[spot] = jnp.sum(update * update, axis=0, keepdims=True)
    new_v[0] = update
    new_v[1] = low
    for to_y in asides:
        for to_x, to_c in (sides[:-1] if to_y is asides[-1] else sides):
            remote(n_v.at[spot], n_v.at[spot], NEAR, (z, to_y, to_x, to_c)).start()

    def others(do):
        def ring(k, carry):
            do(jnp.where(k >= z, k + 1, k))
            return carry
        lax.fori_loop(0, NZ - 1, ring, 0)

    def send_update(to_z):
        for to_y in asides:
            remote(new_v.at[0], u_v.at[sum_f], UPDATE, (to_z, to_y, sum_x, sum_c)).start()

    others(send_update)
    for to_y in asides[:-1]:
        remote(new_v.at[0], u_v.at[sum_f], UPDATE, (z, to_y, sum_x, sum_c)).start()
    home = jnp.logical_and(sum_x == x, sum_c == c)

    @pl.when(home)
    def _():
        pltpu.make_async_copy(new_v.at[0], u_v.at[sum_f], recv_sem.at[UPDATE]).start()

    @pl.when(jnp.logical_not(home))
    def _():
        remote(new_v.at[0], u_v.at[sum_f], UPDATE, (z, y, sum_x, sum_c)).start()

    @pl.when(alone)
    def _():
        pltpu.make_async_copy(new_v.at[1], l_v, recv_sem.at[LOW]).start()

    @pl.when(jnp.logical_not(alone))
    def _():
        remote(new_v.at[1], l_v, LOW, client).start()

    wait_for(n_v.at[pl.ds(0, NY * NT - 1)], recv_sem.at[NEAR])
    g_v[z] = jnp.sum(n_v[...], axis=0)

    @pl.when(c == 1)
    def _():
        def both_cores(to_z):
            for to_c in (0, 1):
                remote(g_v.at[z], g_v.at[z], LINE, (to_z, y, x, to_c)).start()

        others(both_cores)

    wait_for(u_v, recv_sem.at[UPDATE])

    whole = u_v[...].reshape(RANK, DQK)
    high = whole.astype(jnp.bfloat16)
    rest = whole - high.astype(jnp.float32)
    middle = rest.astype(jnp.bfloat16)
    least = (rest - middle.astype(jnp.float32)).astype(jnp.bfloat16)
    basis = b_v[...]
    out_ref[0:32] = (jnp.dot(basis, high, preferred_element_type=jnp.float32)
                     + (jnp.dot(basis, middle, preferred_element_type=jnp.float32)
                        + jnp.dot(basis, least, preferred_element_type=jnp.float32)))
    head_mean = jnp.sum(whole * whole) / (RANK * DQK)

    wait_for(p_v.at[pl.ds(0, NF - 1)], send_sem.at[BASIS])
    for i in range(3):
        wait_for(columns(0), send_sem.at[CROSS + i])
    wait_for(c_v.at[:, pl.ds(0, NX * DQK)], send_sem.at[CORE])

    wait_for(r_v.at[pl.ds(0, NF - 1)], send_sem.at[PARTS])

    @pl.when(home)
    def _():
        wait_for(u_v.at[pl.ds(0, NF - 1)], send_sem.at[UPDATE])

    @pl.when(jnp.logical_not(home))
    def _():
        wait_for(u_v, send_sem.at[UPDATE])

    @pl.when(jnp.logical_not(alone))
    def _():
        wait_for(own_v, send_sem.at[MOMENTS])
        wait_for(l_v, send_sem.at[LOW])

    wait_for(l_v, recv_sem.at[LOW])
    out_ref[32:36] = l_v[...]
    wait_for(n_v.at[pl.ds(0, NY * NT - 1)], send_sem.at[NEAR])
    wait_for(g_v.at[pl.ds(0, NZ - 1)], recv_sem.at[LINE])
    whole_mean = jnp.sum(g_v[...]) / (RANK * HEADS * DQK)
    out_ref[36:40] = jnp.full((4, DQK), head_mean + whole_mean, jnp.float32)

    @pl.when(c == 1)
    def _():
        wait_for(n_v.at[pl.ds(0, 2 * (NZ - 1))], send_sem.at[LINE])


def finish(sums_ref, master_ref, first_ref, second_ref, step_ref, first_out, second_out, copy_ref):
    factor = 1.0 / jnp.sqrt(sums_ref[36:37])
    step = sums_ref[0:32] * factor
    step_ref[...] = step
    copy_ref[...] = (master_ref[...] + step).astype(jnp.bfloat16)
    first_out[...], second_out[...], _ = moments(first_ref[...], second_ref[...], sums_ref[32:36])


def body(inputs, query_cot, query_basis, query_master, query_first, query_second):
    bf16, f32 = jnp.bfloat16, jnp.float32
    sums = pl.pallas_call(
        kernel,
        out_shape=pltpu.VMEM((40, DQK), f32),
        in_specs=[pl.BlockSpec(memory_space=pl.ANY)] * 5,
        out_specs=pl.BlockSpec(memory_space=pltpu.VMEM),
        scratch_shapes=[
            pltpu.VMEM((256, 2048), bf16),
            pltpu.VMEM((256, NT * DQK), bf16),
            pltpu.VMEM((32, RANK), bf16),
            pltpu.VMEM((2, 4, DQK), f32),
            pltpu.VMEM((2, 4, DQK), f32),
            pltpu.VMEM((2, 4, DQK), f32),
            pltpu.VMEM((NF, 8, 128), bf16),
            pltpu.VMEM((8, NT, 4, DQK), f32),
            pltpu.VMEM((NF, 4, DQK), f32),
            pltpu.VMEM((NF, 4, DQK), f32),
            pltpu.VMEM((NY * NT, 1, DQK), f32),
            pltpu.VMEM((NZ, 1, DQK), f32),
            pltpu.VMEM((4, DQK), f32),
            pltpu.SemaphoreType.DMA((5,)),
            pltpu.SemaphoreType.DMA((11,)),
            pltpu.SemaphoreType.DMA((11,)),
        ],
        compiler_params=pltpu.CompilerParams(collective_id=0, has_side_effects=True),
    )(inputs, query_cot, query_basis, query_first, query_second)
    vmem = pl.BlockSpec(memory_space=pltpu.VMEM)
    in_vmem = lambda a: pltpu.with_memory_space_constraint(a, pltpu.VMEM)
    return pl.pallas_call(
        finish,
        out_shape=(jax.ShapeDtypeStruct((32, DQK), f32), jax.ShapeDtypeStruct((4, DQK), f32),
                   jax.ShapeDtypeStruct((4, DQK), f32), jax.ShapeDtypeStruct((32, DQK), bf16)),
        in_specs=[vmem] * 4,
        out_specs=(vmem,) * 4,
    )(in_vmem(sums), in_vmem(query_master), in_vmem(query_first), in_vmem(query_second))


def solution(mesh):
    torus = Mesh(mesh.devices.reshape(NZ, NY, NX, NC), ("z", "y", "x", "c"))
    in_specs = (P(FS, None), P(FS, TP), P(FS, None), P(FS, TP), P(FS, TP), P(FS, TP))
    out_specs = (P(FS, TP), P(FS, TP), P(FS, TP), P(FS, TP))
    return jax.shard_map(body, mesh=torus, in_specs=in_specs, out_specs=out_specs, check_vma=False)
```
